32 devices in a mesh: fs: 16 (over z, y, x), tp: 2 (over core).
Axes of the slice: x: 2, y: 2, z: 4, core: 2. Of those that a mesh axis runs over, the one named last changes fastest.
Arguments:
- saved_inputs: bfloat16 [2048, 4096], P('fs', 'tp'), may hold values from -6 to 6
- value_cotangent: bfloat16 [2048, 2048], P('fs'), may hold values from -0.1875 to 0.1875
- glu_output: bfloat16 [2048, 2048], P('fs', 'tp'), may hold values from -6 to 6
- conv_cotangent: bfloat16 [2048, 2048], P('fs', 'tp'), may hold values from -0.125 to 0.125
- factor: bfloat16 [4096, 256], P('tp'), may hold values from -0.09375 to 0.09375
- value_weight: float32 [2048, 4096], P('fs', 'tp'), may hold values from -3 to 3
- first_moment: float32 [2048, 256], P('fs', 'tp'), may hold values from -6 to 6
- second_moment: float32 [2048, 256], P('fs', 'tp'), may hold values from 0.25 to 4
- kernel: float32 [31, 2048], P(None, 'tp'), may hold values from -1 to 1
- kernel_first: float32 [31, 2048], P(None, 'tp'), may hold values from -6 to 6
- kernel_second: float32 [31, 2048], P(None, 'tp'), may hold values from 0.25 to 4
Outputs:
- new_value: float32 [2048, 4096], P('fs', 'tp')
- value_copy: bfloat16 [2048, 4096], P('fs', 'tp')
- value_step: float32 [2048, 4096], P('fs', 'tp')
- new_first: float32 [2048, 256], P('fs', 'tp')
- new_second: float32 [2048, 256], P('fs', 'tp')
- new_kernel: float32 [31, 2048], P(None, 'tp')
- new_kernel_first: float32 [31, 2048], P(None, 'tp')
- new_kernel_second: float32 [31, 2048], P(None, 'tp')
The draws below stay inside these ranges and needn't reach their ends.
All inputs are finite; a program needn't handle non-finite values.
Results may differ from the reference program's by a relative error of at most 0.0055.
Values may be sent and summed in bfloat16 or wider, within the bound.
No kernel may reach another device: no remote copies, remote signals or barrier semaphores. Data moves between devices by JAX's collectives and lax.ppermute only.
A program may use at most 64 MiB of HBM per device.

```python
import math
import jax
import jax.numpy as jnp
from jax import lax

WIDTH = 4096
CHANNELS = 2048
TAPS = 31
RANK = 256
TOKENS = 2048


def spiked(entries, own_key, source, target, parts, factor):
    def block_of(axis_at):
        return (jnp.arange(entries.shape[axis_at]) // (entries.shape[axis_at] // parts)).reshape((-1,) + (1,) * (entries.ndim - 1 - axis_at))

    first = jax.random.permutation(own_key, parts)[block_of(target)]
    second = (block_of(target) + parts // 2) % parts
    return jnp.where((block_of(source) == first) | (block_of(source) == second), factor * entries, entries)


def shard_levels(rng, dims, split, least, top_value):
    factor_of, own = 1.0, jax.random.fold_in(rng, 6)
    for position, parts in split:
        heights = jnp.exp(jax.random.uniform(jax.random.fold_in(own, position), (parts,), jnp.float32, least / len(split), top_value / len(split)))
        factor_of = factor_of * jnp.repeat(heights, dims[position] // parts).reshape([-1 if axis == position else 1 for axis in range(len(dims))])
    return factor_of


def noise(stream_key, extent, width, limit, shards=(), kind=jnp.bfloat16):
    drawn = width * jax.random.normal(stream_key, extent, jnp.float32)
    if shards:
        drawn = drawn * shard_levels(stream_key, extent, shards, -0.22, 0.18)
    return jnp.clip(drawn, -limit, limit).astype(kind)


def gaussian_with(rng, extent, width, bound, cuts, heavy, dtype=jnp.bfloat16):
    values = width * jax.random.normal(rng, extent, jnp.float32)
    if cuts:
        values = values * shard_levels(rng, extent, cuts, -0.22, 0.18)
    return jnp.clip(spiked(values, jax.random.fold_in(rng, 3), *heavy), -bound, bound).astype(dtype)


def setup_inputs(seed: int = 0) -> dict:
    arg_keys = jax.random.split(jax.random.key(seed), 12)
    saved_inputs = noise(arg_keys[0], (TOKENS, WIDTH), 1.0, 6.0, ((0, 16), (1, 2)))
    value_cotangent = gaussian_with(arg_keys[1], (TOKENS, CHANNELS), (TOKENS ** -0.5), 0.1875, ((0, 16),), (0, 1, 16, 2.0))
    glu_output = noise(arg_keys[2], (TOKENS, CHANNELS), 1.0, 6.0, ((0, 16), (1, 2)))
    conv_cotangent = noise(arg_keys[3], (TOKENS, CHANNELS), (TOKENS ** -0.5), 0.125, ((0, 16), (1, 2)))
    factor = noise(arg_keys[4], (WIDTH, RANK), WIDTH ** -0.5, 0.09375, ((0, 2),))
    value_weight = noise(arg_keys[5], (CHANNELS, WIDTH), 0.5, 3.0, ((0, 16), (1, 2)), jnp.float32)
    first_moment = noise(arg_keys[6], (CHANNELS, RANK), 1.0, 6.0, ((0, 16), (1, 2)), jnp.float32)
    second_moment = jnp.clip(jnp.exp(math.log(4.0) - 2.7725887 * jax.random.uniform(arg_keys[7], (CHANNELS, RANK), jnp.float32) ** shard_levels(arg_keys[7], (CHANNELS, RANK), ((0, 16), (1, 2)), -0.2, 0.2)), 0.25, 4.0)
    kernel = noise(arg_keys[8], (TAPS, CHANNELS), TAPS ** -0.5, 1.0, ((1, 2),), jnp.float32)
    kernel_first = noise(arg_keys[9], (TAPS, CHANNELS), 1.0, 6.0, ((1, 2),), jnp.float32)
    kernel_second = jnp.clip(jnp.exp(math.log(4.0) - 2.7725887 * jax.random.uniform(arg_keys[10], (TAPS, CHANNELS), jnp.float32) ** shard_levels(arg_keys[10], (TAPS, CHANNELS), ((1, 2),), -0.2, 0.2)), 0.25, 4.0)
    return {"saved_inputs": saved_inputs, "value_cotangent": value_cotangent, "glu_output": glu_output, "conv_cotangent": conv_cotangent, "factor": factor, "value_weight": value_weight, "first_moment": first_moment, "second_moment": second_moment, "kernel": kernel, "kernel_first": kernel_first, "kernel_second": kernel_second}


def reference(saved_inputs, value_cotangent, glu_output, conv_cotangent, factor, value_weight, first_moment, second_moment, kernel, kernel_first, kernel_second):
    highest = lax.Precision.HIGHEST
    gradient = jnp.dot(value_cotangent.astype(jnp.float32).T, saved_inputs.astype(jnp.float32), precision=highest, preferred_element_type=jnp.float32)
    factor_f = factor.astype(jnp.float32)
    projected = jnp.dot(gradient, factor_f, precision=highest)
    new_first = 0.8 * first_moment + 0.2 * projected
    new_second = 0.9 * second_moment + 0.1 * projected * projected
    direction = new_first / jnp.sqrt(new_second)
    back_proj = jnp.dot(direction, factor_f.T, precision=highest)
    row_mean = lax.optimization_barrier(jnp.mean(back_proj * back_proj, axis=1, keepdims=True))
    value_step = back_proj / jnp.sqrt(row_mean + 0.01)
    new_value = value_weight - 0.05 * value_step
    value_copy = new_value.astype(jnp.bfloat16)
    padded = jnp.pad(glu_output.astype(jnp.float32), ((TAPS - 1, 0), (0, 0)))
    cotangent_f = conv_cotangent.astype(jnp.float32)
    pieces = []
    for offset in range(TAPS):
        begin = TAPS - 1 - offset
        pieces.append(lax.optimization_barrier(jnp.sum(padded[begin:begin + TOKENS] * cotangent_f, axis=0)))
    kernel_grad = jnp.stack(pieces, axis=0)
    new_kernel_first = 0.8 * kernel_first + 0.2 * kernel_grad
    new_kernel_second = 0.9 * kernel_second + 0.1 * kernel_grad * kernel_grad
    new_kernel = kernel - 0.05 * new_kernel_first / jnp.sqrt(new_kernel_second)
    return (new_value, value_copy, value_step, new_first, new_second, new_kernel, new_kernel_first, new_kernel_second)
```

```python
import jax
import jax.numpy as jnp
from jax import lax
from jax.sharding import PartitionSpec as P

WIDTH = 4096


def from_behind(x, axis, by):
    peers = lax.axis_size(axis)
    pairs = [(i, i + by) for i in range(peers) if 0 <= i + by < peers]
    return lax.ppermute(x, axis, pairs)


def scatter_columns(partial, axis):
    peers = lax.axis_size(axis)
    me = lax.axis_index(axis)
    cols = partial.shape[1] // peers
    total = lax.dynamic_slice_in_dim(partial, me * cols, cols, axis=1)
    for by in range(1, peers):
        target = (me + by) % peers
        block = lax.dynamic_slice_in_dim(partial, target * cols, cols, axis=1)
        pairs = [(i, (i + by) % peers) for i in range(peers)]
        total = total + lax.ppermute(block.astype(jnp.bfloat16), axis, pairs).astype(jnp.float32)
    return total


def sum_peers(x, axis):
    peers = lax.axis_size(axis)
    total = x
    for by in range(1, peers):
        pairs = [(i, (i + by) % peers) for i in range(peers)]
        total = total + lax.ppermute(x, axis, pairs)
    return total


def body(
    saved_inputs,
    value_cotangent,
    glu_output,
    conv_cotangent,
    factor,
    value_weight,
    first_moment,
    second_moment,
    kernel,
    kernel_first,
    kernel_second,
):
    bf16 = jnp.bfloat16
    peers = lax.axis_size("fs")
    taps, channels = kernel.shape

    partial_reduced = jnp.dot(saved_inputs, factor, preferred_element_type=jnp.float32)
    reduced = scatter_columns(partial_reduced, "tp").astype(bf16)
    dims = (((0,), (0,)), ((), ()))
    grad_term = lax.dot_general(value_cotangent, reduced, dims, preferred_element_type=jnp.float32)
    rows = grad_term.shape[0] // peers
    blocks = grad_term.astype(bf16).reshape(peers, rows, grad_term.shape[1])
    received = lax.all_to_all(blocks, "fs", split_axis=0, concat_axis=0, tiled=True)
    projected = jnp.sum(received.astype(jnp.float32), axis=0)

    gram_part = lax.dot_general(factor, factor, dims, preferred_element_type=jnp.float32)
    gram = sum_peers(gram_part, "tp")

    new_first = 0.8 * first_moment + 0.2 * projected
    new_second = 0.9 * second_moment + 0.1 * projected * projected
    direction = new_first / jnp.sqrt(new_second)
    full_direction = lax.all_gather(direction.astype(bf16), "tp", axis=1, tiled=True)
    back_proj = lax.dot_general(
        full_direction, factor, (((1,), (1,)), ((), ())), preferred_element_type=jnp.float32
    )
    wide = full_direction.astype(jnp.float32)
    row_squares = jnp.sum(jnp.dot(wide, gram, precision=lax.Precision.HIGHEST) * wide, axis=1)
    value_step = back_proj * lax.rsqrt(row_squares / WIDTH + 0.01)[:, None]
    new_value = value_weight - 0.05 * value_step
    value_copy = new_value.astype(bf16)

    token_count = glu_output.shape[0]
    reach = taps - 1
    halo_rows = from_behind(glu_output[token_count - reach :], "fs", 1)
    extended = jnp.concatenate([halo_rows, glu_output], axis=0).astype(jnp.float32)
    cotangent_f = conv_cotangent.astype(jnp.float32)
    pieces = []
    for offset in range(taps):
        begin = reach - offset
        pieces.append(jnp.sum(extended[begin : begin + token_count] * cotangent_f, axis=0))
    local_grad = jnp.stack(pieces, axis=0).astype(bf16)
    share = -(-channels * taps // peers)
    share = -(-share // 128) * 128
    flat = jnp.pad(local_grad.reshape(-1), (0, share * peers - taps * channels))
    parts = lax.all_to_all(flat.reshape(peers, share), "fs", split_axis=0, concat_axis=0, tiled=True)
    summed = jnp.sum(parts.astype(jnp.float32), axis=0).astype(bf16)
    gathered = lax.all_gather(summed, "fs", axis=0, tiled=True)
    kernel_grad = gathered[: taps * channels].reshape(taps, channels).astype(jnp.float32)
    new_kernel_first = 0.8 * kernel_first + 0.2 * kernel_grad
    new_kernel_second = 0.9 * kernel_second + 0.1 * kernel_grad * kernel_grad
    new_kernel = kernel - 0.05 * new_kernel_first / jnp.sqrt(new_kernel_second)
    return (
        new_value,
        value_copy,
        value_step,
        new_first,
        new_second,
        new_kernel,
        new_kernel_first,
        new_kernel_second,
    )


def solution(mesh):
    wide = P("fs", "tp")
    taps = P(None, "tp")
    return jax.shard_map(
        body,
        mesh=mesh,
        in_specs=(wide, P("fs", None), wide, wide, P("tp", None), wide, wide, wide, taps, taps, taps),
        out_specs=(wide, wide, wide, wide, wide, taps, taps, taps),
        check_vma=False,
    )
```

```python
import jax
import jax.numpy as jnp
from jax import lax
from jax.experimental import pallas as pl
from jax.experimental.pallas import tpu as pltpu
from jax.sharding import PartitionSpec as P

WIDTH = 4096


def from_behind(x, axis, by):
    peers = lax.axis_size(axis)
    pairs = [(i, i + by) for i in range(peers) if 0 <= i + by < peers]
    return lax.ppermute(x, axis, pairs)


def scatter_columns(partial, axis):
    peers = lax.axis_size(axis)
    me = lax.axis_index(axis)
    cols = partial.shape[1] // peers
    total = lax.dynamic_slice_in_dim(partial, me * cols, cols, axis=1)
    for by in range(1, peers):
        target = (me + by) % peers
        block = lax.dynamic_slice_in_dim(partial, target * cols, cols, axis=1)
        pairs = [(i, (i + by) % peers) for i in range(peers)]
        total = total + lax.ppermute(block.astype(jnp.bfloat16), axis, pairs).astype(jnp.float32)
    return total


def sum_peers(x, axis):
    peers = lax.axis_size(axis)
    total = x
    for by in range(1, peers):
        pairs = [(i, (i + by) % peers) for i in range(peers)]
        total = total + lax.ppermute(x, axis, pairs)
    return total


LANES = 128
SUB = 16


def rounded(n, to):
    return -(-n // to) * to


def tap_sums(halo, tokens, cotangent, taps):
    count, channels = tokens.shape
    tiles = channels // LANES
    reach = halo.shape[0]
    depth = rounded(taps, SUB)

    def run(halo_ref, tokens_ref, cot_ref, out_ref, ext_ref, sums_ref):
        sums_ref[...] = jnp.zeros_like(sums_ref)

        def tile(l, carry):
            lanes = pl.ds(pl.multiple_of(l * LANES, LANES), LANES)
            ext_ref[pl.ds(0, reach), :] = halo_ref[:, lanes].astype(jnp.float32)
            ext_ref[pl.ds(reach, count), :] = tokens_ref[:, lanes].astype(jnp.float32)
            cot = cot_ref[:, lanes].astype(jnp.float32)
            for k in range(taps):
                window = ext_ref[pl.ds(reach - k, count), :]
                sums_ref[pl.ds(k, 1), :] = jnp.sum(window * cot, axis=0, keepdims=True)
            rows = pl.ds(pl.multiple_of(l * depth, depth), depth)
            out_ref[rows, :] = sums_ref[...].astype(out_ref.dtype)
            return carry

        lax.fori_loop(0, tiles, tile, 0)

    return pl.pallas_call(
        run,
        out_shape=jax.ShapeDtypeStruct((tiles * depth, LANES), jnp.bfloat16),
        scratch_shapes=[
            pltpu.VMEM((reach + count, LANES), jnp.float32),
            pltpu.VMEM((depth, LANES), jnp.float32),
        ],
        name="tap_sums",
    )(halo, tokens, cotangent)


def packed_blocks(reduced, cotangent, share, peers):
    cols = reduced.shape[1]
    rows = cotangent.shape[1] // peers
    dims = (((0,), (0,)), ((), ()))
    extra = share.shape[1]
    if rows % LANES or cols % SUB or extra % SUB:
        term = lax.dot_general(reduced, cotangent, dims, preferred_element_type=jnp.float32)
        term = term.astype(jnp.bfloat16).reshape(cols, peers, rows).transpose(1, 0, 2)
        return jnp.concatenate([term, share], axis=1)

    def run(reduced_ref, cot_ref, share_ref, out_ref):
        term = lax.dot_general(
            reduced_ref[...], cot_ref[...], dims, preferred_element_type=jnp.float32
        )
        for p in range(peers):
            out_ref[p, :cols, :] = term[:, p * rows : (p + 1) * rows].astype(out_ref.dtype)
            out_ref[p, cols:, :] = share_ref[p]

    return pl.pallas_call(
        run,
        out_shape=jax.ShapeDtypeStruct((peers, cols + extra, rows), jnp.bfloat16),
        name="packed_blocks",
    )(reduced, cotangent, share)


def updated_taps(grads, kernel, kernel_first, kernel_second):
    taps, channels = kernel.shape
    tiles = channels // LANES
    depth = grads.shape[0] // tiles

    def run(grads_ref, kernel_ref, first_ref, second_ref, out_ref, out_first_ref, out_second_ref):
        for l in range(tiles):
            lanes = pl.ds(l * LANES, LANES)
            grad = grads_ref[pl.ds(l * depth, depth), :].astype(jnp.float32)[:taps]
            first = 0.8 * first_ref[:, lanes] + 0.2 * grad
            second = 0.9 * second_ref[:, lanes] + 0.1 * grad * grad
            out_first_ref[:, lanes] = first
            out_second_ref[:, lanes] = second
            out_ref[:, lanes] = kernel_ref[:, lanes] - 0.05 * first * lax.rsqrt(second)

    like = jax.ShapeDtypeStruct(kernel.shape, jnp.float32)
    return pl.pallas_call(run, out_shape=(like, like, like), name="updated_taps")(
        grads, kernel, kernel_first, kernel_second
    )


def body(
    saved_inputs,
    value_cotangent,
    glu_output,
    conv_cotangent,
    factor,
    value_weight,
    first_moment,
    second_moment,
    kernel,
    kernel_first,
    kernel_second,
):
    bf16 = jnp.bfloat16
    peers = lax.axis_size("fs")
    taps = kernel.shape[0]
    token_count = glu_output.shape[0]

    reach = rounded(taps - 1, SUB)
    halo_rows = from_behind(glu_output[token_count - reach :], "fs", 1)
    local_grad = tap_sums(halo_rows, glu_output, conv_cotangent, taps)

    partial_reduced = jnp.dot(saved_inputs, factor, preferred_element_type=jnp.float32)
    reduced = scatter_columns(partial_reduced, "tp").astype(bf16)
    cols = reduced.shape[1]
    rows = value_cotangent.shape[1] // peers
    share = local_grad.reshape(peers, -1, rows)
    blocks = packed_blocks(reduced, value_cotangent, share, peers)
    received = lax.all_to_all(blocks, "fs", split_axis=0, concat_axis=0, tiled=True)
    share_sum = jnp.sum(received[:, cols:].astype(jnp.float32), axis=0).astype(bf16)
    projected = jnp.sum(received[:, :cols].astype(jnp.float32), axis=0).T

    copies = jnp.broadcast_to(share_sum[None], share.shape)
    grads = lax.all_to_all(copies, "fs", split_axis=0, concat_axis=0, tiled=True)

    dims = (((0,), (0,)), ((), ()))
    gram_part = lax.dot_general(factor, factor, dims, preferred_element_type=jnp.float32)
    gram = sum_peers(gram_part, "tp")

    new_first = 0.8 * first_moment + 0.2 * projected
    new_second = 0.9 * second_moment + 0.1 * projected * projected
    direction = new_first * lax.rsqrt(new_second)
    full_direction = lax.all_gather(direction.astype(bf16), "tp", axis=1, tiled=True)
    back_proj = lax.dot_general(
        full_direction, factor, (((1,), (1,)), ((), ())), preferred_element_type=jnp.float32
    )
    wide = full_direction.astype(jnp.float32)
    row_squares = jnp.sum(jnp.dot(wide, gram, precision=lax.Precision.HIGHEST) * wide, axis=1)
    value_step = back_proj * lax.rsqrt(row_squares / WIDTH + 0.01)[:, None]
    new_value = value_weight - 0.05 * value_step
    value_copy = new_value.astype(bf16)

    new_kernel, new_kernel_first, new_kernel_second = updated_taps(
        grads.reshape(local_grad.shape), kernel, kernel_first, kernel_second
    )
    return (
        new_value,
        value_copy,
        value_step,
        new_first,
        new_second,
        new_kernel,
        new_kernel_first,
        new_kernel_second,
    )


def solution(mesh):
    wide = P("fs", "tp")
    taps = P(None, "tp")
    return jax.shard_map(
        body,
        mesh=mesh,
        in_specs=(wide, P("fs", None), wide, wide, P("tp", None), wide, wide, wide, taps, taps, taps),
        out_specs=(wide, wide, wide, wide, wide, taps, taps, taps),
        check_vma=False,
    )
```

```python
import jax
import jax.numpy as jnp
from jax import lax
from jax.experimental import pallas as pl
from jax.experimental.pallas import tpu as pltpu
from jax.sharding import PartitionSpec as P


WIDTH = 4096


def from_behind(x, axis, by):
    peers = lax.axis_size(axis)
    pairs = [(i, i + by) for i in range(peers) if 0 <= i + by < peers]
    return lax.ppermute(x, axis, pairs)


def scatter_columns(partial, axis):
    peers = lax.axis_size(axis)
    me = lax.axis_index(axis)
    cols = partial.shape[1] // peers
    total = lax.dynamic_slice_in_dim(partial, me * cols, cols, axis=1)
    for by in range(1, peers):
        target = (me + by) % peers
        block = lax.dynamic_slice_in_dim(partial, target * cols, cols, axis=1)
        pairs = [(i, (i + by) % peers) for i in range(peers)]
        total = total + lax.ppermute(block.astype(jnp.bfloat16), axis, pairs).astype(jnp.float32)
    return total


def sum_peers(x, axis):
    peers = lax.axis_size(axis)
    total = x
    for by in range(1, peers):
        pairs = [(i, (i + by) % peers) for i in range(peers)]
        total = total + lax.ppermute(x, axis, pairs)
    return total


LANES = 128
SUB = 16


def rounded(n, to):
    return -(-n // to) * to


def exchange(x, groups):
    return lax.all_to_all(
        x, "fs", split_axis=0, concat_axis=0, tiled=True, axis_index_groups=groups
    )


def on_chip(*arrays):
    return tuple(pltpu.with_memory_space_constraint(x, pltpu.VMEM) for x in arrays)


def tap_sums(halo, tokens, cotangent, taps):
    count, channels = tokens.shape
    tiles = channels // LANES
    reach = halo.shape[0]
    depth = rounded(taps, SUB)

    def run(halo_ref, tokens_ref, cot_ref, out_ref, ext_ref, sums_ref):
        sums_ref[...] = jnp.zeros_like(sums_ref)

        def tile(l, carry):
            lanes = pl.ds(pl.multiple_of(l * LANES, LANES), LANES)
            ext_ref[pl.ds(0, reach), :] = halo_ref[:, lanes].astype(jnp.float32)
            ext_ref[pl.ds(reach, count), :] = tokens_ref[:, lanes].astype(jnp.float32)
            cot = cot_ref[:, lanes].astype(jnp.float32)
            for k in range(taps):
                window = ext_ref[pl.ds(reach - k, count), :]
                sums_ref[pl.ds(k, 1), :] = jnp.sum(window * cot, axis=0, keepdims=True)
            rows = pl.ds(pl.multiple_of(l * depth, depth), depth)
            out_ref[rows, :] = sums_ref[...].astype(out_ref.dtype)
            return carry

        lax.fori_loop(0, tiles, tile, 0)

    return pl.pallas_call(
        run,
        out_shape=pltpu.VMEM((tiles * depth, LANES), jnp.bfloat16),
        scratch_shapes=[
            pltpu.VMEM((reach + count, LANES), jnp.float32),
            pltpu.VMEM((depth, LANES), jnp.float32),
        ],
        name="tap_sums",
    )(*on_chip(halo, tokens, cotangent))


def packed_blocks(reduced, cotangent, share, peers, near):
    cols = reduced.shape[1]
    rows = cotangent.shape[1] // peers
    far = peers // near
    dims = (((0,), (0,)), ((), ()))
    extra = share.shape[1]
    if rows % LANES or cols % SUB or extra % SUB:
        term = lax.dot_general(reduced, cotangent, dims, preferred_element_type=jnp.float32)
        term = term.astype(jnp.bfloat16).reshape(cols, far, near, rows)
        term = term.transpose(2, 1, 0, 3).reshape(near, far * cols, rows)
        return jnp.concatenate([term, share], axis=1)

    def run(reduced_ref, cot_ref, share_ref, out_ref):
        term = lax.dot_general(
            reduced_ref[...], cot_ref[...], dims, preferred_element_type=jnp.float32
        )
        for f in range(far):
            for n in range(near):
                p = f * near + n
                block = term[:, p * rows : (p + 1) * rows].astype(out_ref.dtype)
                out_ref[n, f * cols : (f + 1) * cols, :] = block
        for n in range(near):
            out_ref[n, far * cols :, :] = share_ref[n]

    return pl.pallas_call(
        run,
        out_shape=jax.ShapeDtypeStruct((near, far * cols + extra, rows), jnp.bfloat16),
        name="packed_blocks",
    )(*on_chip(reduced, cotangent, share))


def updated_taps(grads, kernel, kernel_first, kernel_second):
    taps, channels = kernel.shape
    tiles = channels // LANES
    depth = grads.shape[0] // tiles

    def run(grads_ref, kernel_ref, first_ref, second_ref, out_ref, out_first_ref, out_second_ref):
        for l in range(tiles):
            lanes = pl.ds(l * LANES, LANES)
            grad = grads_ref[pl.ds(l * depth, depth), :].astype(jnp.float32)[:taps]
            first = 0.8 * first_ref[:, lanes] + 0.2 * grad
            second = 0.9 * second_ref[:, lanes] + 0.1 * grad * grad
            out_first_ref[:, lanes] = first
            out_second_ref[:, lanes] = second
            out_ref[:, lanes] = kernel_ref[:, lanes] - 0.05 * first * lax.rsqrt(second)

    like = jax.ShapeDtypeStruct(kernel.shape, jnp.float32)
    return pl.pallas_call(run, out_shape=(like, like, like), name="updated_taps")(
        *on_chip(grads, kernel, kernel_first, kernel_second)
    )


def body(
    saved_inputs,
    value_cotangent,
    glu_output,
    conv_cotangent,
    factor,
    value_weight,
    first_moment,
    second_moment,
    kernel,
    kernel_first,
    kernel_second,
):
    bf16 = jnp.bfloat16
    peers = lax.axis_size("fs")
    taps = kernel.shape[0]
    token_count = glu_output.shape[0]

    reach = rounded(taps - 1, SUB)
    halo_rows = from_behind(glu_output[token_count - reach :], "fs", 1)
    local_grad = tap_sums(halo_rows, glu_output, conv_cotangent, taps)

    partial_reduced = jnp.dot(saved_inputs, factor, preferred_element_type=jnp.float32)
    reduced = scatter_columns(partial_reduced, "tp").astype(bf16)
    cols = reduced.shape[1]
    rows = value_cotangent.shape[1] // peers
    near = 4 if peers % 4 == 0 else 1
    far = peers // near
    groups = [[f * near + n for n in range(near)] for f in range(far)]
    across = [[f * near + n for f in range(far)] for n in range(near)]
    share = local_grad.reshape(near, -1, rows)
    blocks = packed_blocks(reduced, value_cotangent, share, peers, near)
    received = exchange(blocks, groups)
    summed = jnp.sum(received.astype(jnp.float32), axis=0).astype(bf16)
    main = summed[: far * cols].reshape(far, cols, rows)
    taps_part = jnp.broadcast_to(summed[far * cols :][None], (far,) + share.shape[1:])
    received = exchange(jnp.concatenate([main, taps_part], axis=1), across)
    total = jnp.sum(received.astype(jnp.float32), axis=0)
    projected = total[:cols].T

    copies = jnp.broadcast_to(total[cols:].astype(bf16)[None], share.shape)
    grads = exchange(copies, groups)

    dims = (((0,), (0,)), ((), ()))
    gram_part = lax.dot_general(factor, factor, dims, preferred_element_type=jnp.float32)
    gram = sum_peers(gram_part, "tp")

    new_first = 0.8 * first_moment + 0.2 * projected
    new_second = 0.9 * second_moment + 0.1 * projected * projected
    direction = new_first * lax.rsqrt(new_second)
    full_direction = lax.all_gather(direction.astype(bf16), "tp", axis=1, tiled=True)
    back_proj = lax.dot_general(
        full_direction, factor, (((1,), (1,)), ((), ())), preferred_element_type=jnp.float32
    )
    wide = full_direction.astype(jnp.float32)
    row_squares = jnp.sum(jnp.dot(wide, gram, precision=lax.Precision.HIGHEST) * wide, axis=1)
    value_step = back_proj * lax.rsqrt(row_squares / WIDTH + 0.01)[:, None]
    new_value = value_weight - 0.05 * value_step
    value_copy = new_value.astype(bf16)

    new_kernel, new_kernel_first, new_kernel_second = updated_taps(
        grads.reshape(local_grad.shape), kernel, kernel_first, kernel_second
    )
    return (
        new_value,
        value_copy,
        value_step,
        new_first,
        new_second,
        new_kernel,
        new_kernel_first,
        new_kernel_second,
    )


def solution(mesh):
    wide = P("fs", "tp")
    taps = P(None, "tp")
    return jax.shard_map(
        body,
        mesh=mesh,
        in_specs=(wide, P("fs", None), wide, wide, P("tp", None), wide, wide, wide, taps, taps, taps),
        out_specs=(wide, wide, wide, wide, wide, taps, taps, taps),
        check_vma=False,
    )
```

```python
import jax
import jax.numpy as jnp
from jax import lax
from jax.experimental import pallas as pl
from jax.experimental.pallas import tpu as pltpu
from jax.sharding import PartitionSpec as P


WIDTH = 4096


def from_behind(x, axis, by):
    peers = lax.axis_size(axis)
    pairs = [(i, i + by) for i in range(peers) if 0 <= i + by < peers]
    return lax.ppermute(x, axis, pairs)


def scatter_columns(partial, axis):
    peers = lax.axis_size(axis)
    me = lax.axis_index(axis)
    cols = partial.shape[1] // peers
    total = lax.dynamic_slice_in_dim(partial, me * cols, cols, axis=1)
    for by in range(1, peers):
        target = (me + by) % peers
        block = lax.dynamic_slice_in_dim(partial, target * cols, cols, axis=1)
        pairs = [(i, (i + by) % peers) for i in range(peers)]
        total = total + lax.ppermute(block.astype(jnp.bfloat16), axis, pairs).astype(jnp.float32)
    return total


def sum_peers(x, axis):
    peers = lax.axis_size(axis)
    total = x
    for by in range(1, peers):
        pairs = [(i, (i + by) % peers) for i in range(peers)]
        total = total + lax.ppermute(x, axis, pairs)
    return total


LANES = 128
SUB = 16


def rounded(n, to):
    return -(-n // to) * to


def on_chip(*arrays):
    return tuple(pltpu.with_memory_space_constraint(x, pltpu.VMEM) for x in arrays)


def tap_sums(halo, tokens, cotangent, taps):
    count, channels = tokens.shape
    tiles = channels // LANES
    reach = halo.shape[0]
    depth = rounded(taps, SUB)

    def run(halo_ref, tokens_ref, cot_ref, out_ref, ext_ref, sums_ref):
        sums_ref[...] = jnp.zeros_like(sums_ref)

        def tile(l, carry):
            lanes = pl.ds(pl.multiple_of(l * LANES, LANES), LANES)
            ext_ref[pl.ds(0, reach), :] = halo_ref[:, lanes].astype(jnp.float32)
            ext_ref[pl.ds(reach, count), :] = tokens_ref[:, lanes].astype(jnp.float32)
            cot = cot_ref[:, lanes].astype(jnp.float32)
            for k in range(taps):
                window = ext_ref[pl.ds(reach - k, count), :]
                sums_ref[pl.ds(k, 1), :] = jnp.sum(window * cot, axis=0, keepdims=True)
            rows = pl.ds(pl.multiple_of(l * depth, depth), depth)
            out_ref[rows, :] = sums_ref[...].astype(out_ref.dtype)
            return carry

        lax.fori_loop(0, tiles, tile, 0)

    return pl.pallas_call(
        run,
        out_shape=pltpu.VMEM((tiles * depth, LANES), jnp.bfloat16),
        scratch_shapes=[
            pltpu.VMEM((reach + count, LANES), jnp.float32),
            pltpu.VMEM((depth, LANES), jnp.float32),
        ],
        name="tap_sums",
    )(*on_chip(halo, tokens, cotangent))


def row_blocks(reduced, cotangent, peers):
    cols = reduced.shape[1]
    rows = cotangent.shape[1] // peers
    dims = (((0,), (0,)), ((), ()))
    if rows % LANES or cols % SUB:
        term = lax.dot_general(reduced, cotangent, dims, preferred_element_type=jnp.float32)
        return term.astype(jnp.bfloat16).reshape(cols, peers, rows).transpose(1, 0, 2)

    def run(reduced_ref, cot_ref, out_ref):
        term = lax.dot_general(
            reduced_ref[...], cot_ref[...], dims, preferred_element_type=jnp.float32
        )
        for p in range(peers):
            out_ref[p] = term[:, p * rows : (p + 1) * rows].astype(out_ref.dtype)

    return pl.pallas_call(
        run,
        out_shape=jax.ShapeDtypeStruct((peers, cols, rows), jnp.bfloat16),
        name="row_blocks",
    )(*on_chip(reduced, cotangent))


def collected(x, axis, place, count, pairs_by):
    out = lax.dynamic_update_index_in_dim(jnp.zeros((count,) + x.shape, x.dtype), x, place, 0)
    for by in range(1, count):
        got = lax.ppermute(x, axis, pairs_by(by))
        out = lax.dynamic_update_index_in_dim(out, got, (place - by) % count, 0)
    return out


def summed_taps(local, axis):
    peers = lax.axis_size(axis)
    near = 4 if peers % 4 == 0 else 1
    far = peers // near
    me = lax.axis_index(axis)
    n, f = me % near, me // near

    def inside(by):
        return [(g * near + i, g * near + (i + by) % near) for g in range(far) for i in range(near)]

    def across(by):
        return [(g * near + i, (g + by) % far * near + i) for g in range(far) for i in range(near)]

    parts = local.reshape(near, -1, local.shape[1])
    total = lax.dynamic_index_in_dim(parts, n, 0, keepdims=False).astype(jnp.float32)
    for by in range(1, near):
        block = lax.dynamic_index_in_dim(parts, (n + by) % near, 0, keepdims=False)
        total = total + lax.ppermute(block, axis, inside(by)).astype(jnp.float32)
    sums = collected(total.astype(local.dtype), axis, f, far, across)
    total = jnp.sum(sums.astype(jnp.float32), axis=0).astype(local.dtype)
    return collected(total, axis, n, near, inside).reshape(local.shape)


def updated_taps(grads, kernel, kernel_first, kernel_second):
    taps, channels = kernel.shape
    tiles = channels // LANES
    depth = grads.shape[0] // tiles

    def run(grads_ref, kernel_ref, first_ref, second_ref, out_ref, out_first_ref, out_second_ref):
        for l in range(tiles):
            lanes = pl.ds(l * LANES, LANES)
            grad = grads_ref[pl.ds(l * depth, depth), :].astype(jnp.float32)[:taps]
            first = 0.8 * first_ref[:, lanes] + 0.2 * grad
            second = 0.9 * second_ref[:, lanes] + 0.1 * grad * grad
            out_first_ref[:, lanes] = first
            out_second_ref[:, lanes] = second
            out_ref[:, lanes] = kernel_ref[:, lanes] - 0.05 * first * lax.rsqrt(second)

    like = jax.ShapeDtypeStruct(kernel.shape, jnp.float32)
    return pl.pallas_call(run, out_shape=(like, like, like), name="updated_taps")(
        *on_chip(grads, kernel, kernel_first, kernel_second)
    )


def body(
    saved_inputs,
    value_cotangent,
    glu_output,
    conv_cotangent,
    factor,
    value_weight,
    first_moment,
    second_moment,
    kernel,
    kernel_first,
    kernel_second,
):
    bf16 = jnp.bfloat16
    peers = lax.axis_size("fs")
    taps = kernel.shape[0]
    token_count = glu_output.shape[0]

    reach = rounded(taps - 1, SUB)
    halo_rows = from_behind(glu_output[token_count - reach :], "fs", 1)
    local_grad = tap_sums(halo_rows, glu_output, conv_cotangent, taps)

    partial_reduced = jnp.dot(saved_inputs, factor, preferred_element_type=jnp.float32)
    reduced = scatter_columns(partial_reduced, "tp").astype(bf16)
    blocks = row_blocks(reduced, value_cotangent, peers)
    received = lax.all_to_all(blocks, "fs", split_axis=0, concat_axis=0, tiled=True)
    projected = jnp.sum(received.astype(jnp.float32), axis=0).T

    dims = (((0,), (0,)), ((), ()))
    gram_part = lax.dot_general(factor, factor, dims, preferred_element_type=jnp.float32)
    gram = sum_peers(gram_part, "tp")

    new_first = 0.8 * first_moment + 0.2 * projected
    new_second = 0.9 * second_moment + 0.1 * projected * projected
    direction = new_first * lax.rsqrt(new_second)
    full_direction = lax.all_gather(direction.astype(bf16), "tp", axis=1, tiled=True)
    back_proj = lax.dot_general(
        full_direction, factor, (((1,), (1,)), ((), ())), preferred_element_type=jnp.float32
    )
    wide = full_direction.astype(jnp.float32)
    row_squares = jnp.sum(jnp.dot(wide, gram, precision=lax.Precision.HIGHEST) * wide, axis=1)
    value_step = back_proj * lax.rsqrt(row_squares / WIDTH + 0.01)[:, None]
    new_value = value_weight - 0.05 * value_step
    value_copy = new_value.astype(bf16)

    grads = summed_taps(local_grad, "fs")
    new_kernel, new_kernel_first, new_kernel_second = updated_taps(
        grads, kernel, kernel_first, kernel_second
    )
    return (
        new_value,
        value_copy,
        value_step,
        new_first,
        new_second,
        new_kernel,
        new_kernel_first,
        new_kernel_second,
    )


def solution(mesh):
    wide = P("fs", "tp")
    taps = P(None, "tp")
    return jax.shard_map(
        body,
        mesh=mesh,
        in_specs=(wide, P("fs", None), wide, wide, P("tp", None), wide, wide, wide, taps, taps, taps),
        out_specs=(wide, wide, wide, wide, wide, taps, taps, taps),
        check_vma=False,
    )
```
